32 devices in a mesh: grp: 1, sp: 16 (over z, y, core), tp: 2 (over x).
Axes of the slice: x: 2, y: 2, z: 4, core: 2. Of those that a mesh axis runs over, the one named last changes fastest.
Arguments:
- residual_in: bfloat16 [2048, 2048], P(('grp', 'sp'), 'tp'), may hold values from -16 to 16
- query_pre: bfloat16 [2048, 512], P(('grp', 'sp'), 'tp'), may hold values from -6 to 6
- forget_pre: bfloat16 [2048, 512], P(('grp', 'sp'), 'tp'), may hold values from -9 to 9
- value_pre: bfloat16 [2048, 512], P(('grp', 'sp'), 'tp'), may hold values from -6 to 6
- gate_pre: bfloat16 [2048, 512], P(('grp', 'sp'), 'tp'), may hold values from -6 to 6
- floor_gap: float32 [512], P('tp'), may hold values from 0 to 1, as said below
- head_gain: float32 [64], replicated, may hold values from 0.1 to 1.9
- out_weight: bfloat16 [512, 2048], P(None, 'tp'), may hold values from -0.25 to 0.25
- norm_gain: float32 [2048], P('tp'), may hold values from 0.1 to 1.9
- value_weight: bfloat16 [2048, 5632], P('sp', 'tp'), may hold values from -0.125 to 0.125
- gate_weight: bfloat16 [2048, 5632], P('sp', 'tp'), may hold values from -0.125 to 0.125
- value_taps: float32 [3, 5632], P(None, 'tp'), may hold values from -3 to 3
- gate_taps: float32 [3, 5632], P(None, 'tp'), may hold values from -3 to 3
- down_weight: bfloat16 [5632, 2048], P('tp', 'sp'), may hold values from -0.078125 to 0.078125
Outputs:
- mixed: bfloat16 [2048, 2048], P(('grp', 'sp'), 'tp')
The draws below stay inside these ranges and needn't reach their ends.
Inputs may be any that keep to these rules, and one draw needn't show every extreme that they name: `floor_gap`: each channel's value lies strictly between 0 and 1.
All inputs are finite; a program needn't handle non-finite values.
Results may differ from the reference program's by a relative error of at most 0.0085.
Values may be sent and summed in bfloat16 or wider, within the bound.
A program may use at most 128 MiB of HBM per device.

```python
import jax
import jax.numpy as jnp
from jax import lax

D = 2048
H = 8
DK = 64
DV = 64
FF = 5632
TAPS = 3
BLOCK = 64
TOK_DEV = 128
TOKENS = 2048


def draw_residual_in(key, part):
    noise_key, order_key = jax.random.split(jax.random.fold_in(key, 11))
    base = jax.random.normal(noise_key, (TOKENS, D), jnp.float32)
    ranking = jax.random.permutation(order_key, 4).astype(jnp.float32)
    scales = 0.35 * 6.0 ** (ranking / 3.0)
    return (base.reshape(TOKENS, 4, D // 4) * scales[None, :, None]).reshape(TOKENS, D).astype(jnp.bfloat16)


def draw_forget_pre(key, part):
    noise_key, offset_key = jax.random.split(jax.random.fold_in(key, 17))
    base = jnp.clip(jax.random.normal(noise_key, (TOKENS, H * DK), jnp.float32), -6.0, 6.0)
    offsets = jax.random.uniform(offset_key, (TOKENS // TOK_DEV, 1, H * DK), jnp.float32, -1.5, 1.5)
    return (base.reshape(TOKENS // TOK_DEV, TOK_DEV, H * DK) + offsets).reshape(TOKENS, H * DK).astype(jnp.bfloat16)


def draw_floor_gap(key, part):
    order_key, slow_key, fast_key = jax.random.split(jax.random.fold_in(key, 23), 3)
    ranking = jax.random.permutation(order_key, H)
    quick = ranking < H // 2
    slow_values = jnp.exp(jax.random.uniform(slow_key, (H, DK), jnp.float32, jnp.log(0.3 / TOKENS), jnp.log(2.5 / TOKENS)))
    fast_values = jnp.exp(jax.random.uniform(fast_key, (H, DK), jnp.float32, jnp.log(0.02), jnp.log(0.06)))
    return jnp.where(quick[:, None], fast_values, slow_values).reshape(H * DK)


def shard_levels(rng, dims, cuts, least, largest):
    gain, own = 1.0, jax.random.fold_in(rng, 6)
    for dim, blocks in cuts:
        heights = jnp.exp(jax.random.uniform(jax.random.fold_in(own, dim), (blocks,), jnp.float32, least / len(cuts), largest / len(cuts)))
        gain = gain * jnp.repeat(heights, dims[dim] // blocks).reshape([-1 if axis == dim else 1 for axis in range(len(dims))])
    return gain


def centred(rng, extent, scale, reach, shards=(), kind=jnp.bfloat16):
    factor_of = shard_levels(rng, extent, shards, -0.22, 0.18) if shards else 1.0
    values = jax.random.normal(rng, extent, jnp.float32) * scale * factor_of
    return jnp.minimum(jnp.maximum(values, -reach), reach).astype(kind)


def setup_inputs(seed: int = 0, part: int = 0) -> dict:
    streams_of = jax.random.split(jax.random.key(seed), 15)
    part_keys = jax.random.split(jax.random.fold_in(streams_of[14], part), 15)
    return {
        "residual_in": draw_residual_in(jax.random.fold_in(jax.random.fold_in(streams_of[14], part), 71), part),
        "query_pre": centred(part_keys[1], (TOKENS, H * DK), 1.0, 6.0, ((0, 16), (1, 2))),
        "forget_pre": draw_forget_pre(jax.random.fold_in(jax.random.fold_in(streams_of[14], part), 71), part),
        "value_pre": centred(part_keys[3], (TOKENS, H * DV), 1.0, 6.0, ((0, 16), (1, 2))),
        "gate_pre": centred(part_keys[4], (TOKENS, H * DV), 1.0, 6.0, ((0, 16), (1, 2))),
        "floor_gap": draw_floor_gap(jax.random.fold_in(streams_of[14], 71), part),
        "head_gain": jnp.clip(1.0 + 0.18 * jax.random.normal(streams_of[6], (DV,), jnp.float32), 0.1, 1.9),
        "out_weight": centred(streams_of[7], (H * DV, D), (H * DV) ** -0.5, 0.25, ((1, 2),)),
        "norm_gain": jnp.clip(1.0 + 0.18 * jax.random.normal(streams_of[8], (D,), jnp.float32), 0.1, 1.9),
        "value_weight": centred(streams_of[9], (D, FF), D ** -0.5, 0.125, ((0, 16), (1, 2))),
        "gate_weight": centred(streams_of[10], (D, FF), D ** -0.5, 0.125, ((0, 16), (1, 2))),
        "value_taps": centred(streams_of[11], (TAPS, FF), 0.577, 3.0, ((1, 2),), jnp.float32),
        "gate_taps": centred(streams_of[12], (TAPS, FF), 0.577, 3.0, ((1, 2),), jnp.float32),
        "down_weight": centred(streams_of[13], (FF, D), FF ** -0.5, 0.078125, ((0, 2), (1, 16))),
    }


epsilon = 1e-06
highest_precision = lax.Precision.HIGHEST

def split_heads(matrix, head_count):
    return matrix.reshape(matrix.shape[0], head_count, -1).transpose(1, 0, 2)

def recurrence(query_rows, gate_keys, values, log_decay, block_size, start_state):
    head_count, seq_length, key_width = query_rows.shape
    block_count = seq_length // block_size

    def to_blocks(tensor):
        return tensor.reshape(head_count, block_count, block_size, tensor.shape[-1]).transpose(1, 0, 2, 3)
    causal = jnp.tril(jnp.ones((block_size, block_size), dtype=bool))

    def advance(current_state, inputs):
        block_queries, block_keys, block_values, decay_block = inputs
        running_state = jnp.cumsum(decay_block, axis=1)
        carried_state = jnp.einsum('pen,pnd->ped', block_queries * jnp.exp(running_state), current_state, precision=highest_precision)
        spread = jnp.where(causal[None, :, :, None], running_state[:, :, None, :] - running_state[:, None, :, :], -jnp.inf)
        scores = jnp.einsum('htk,hsk,htsk->hts', block_queries, block_keys, jnp.exp(spread), precision=highest_precision)
        inner = jnp.einsum('hts,hsv->htv', scores, block_values, precision=highest_precision)
        ending_state = running_state[:, -1, :]
        fresh_update = jnp.einsum('bia,big->bag', block_keys * jnp.exp(ending_state[:, None, :] - running_state), block_values, precision=highest_precision)
        return (jnp.exp(ending_state)[:, :, None] * current_state + fresh_update, carried_state + inner)
    final_state, outputs = lax.scan(advance, start_state, (to_blocks(query_rows), to_blocks(gate_keys), to_blocks(values), to_blocks(log_decay)))
    return (final_state, outputs.transpose(1, 0, 2, 3).reshape(head_count, seq_length, values.shape[-1]))

def mixer_inputs(query_pre, forget_pre, value_pre, floor_gap, head_count):
    gate_keys = floor_gap.astype(jnp.float32) * jax.nn.sigmoid(-forget_pre.astype(jnp.float32))
    log_decay = jnp.log1p(-gate_keys)
    query_rows = jax.nn.silu(query_pre.astype(jnp.float32))
    return (split_heads(query_rows, head_count), split_heads(gate_keys, head_count), split_heads(value_pre.astype(jnp.float32), head_count), split_heads(log_decay, head_count))

def head_output(recurrent, head_gain, gate_pre):
    ordered = recurrent.transpose(1, 0, 2)
    scaled = ordered * lax.rsqrt(lax.optimization_barrier(jnp.mean(ordered * ordered, axis=-1, keepdims=True)) + epsilon) * head_gain
    gating = jax.nn.silu(gate_pre.astype(jnp.float32)).reshape(ordered.shape)
    return (scaled * gating).reshape(ordered.shape[0], -1).astype(jnp.bfloat16)

def causal_taps(padded, taps, row_count):
    return taps[0] * padded[0:row_count] + taps[1] * padded[1:row_count + 1] + taps[2] * padded[2:row_count + 2]

def reference(residual_in, query_pre, forget_pre, value_pre, gate_pre, floor_gap, head_gain, out_weight, norm_gain, value_weight, gate_weight, value_taps, gate_taps, down_weight):
    row_count = residual_in.shape[0]
    query_rows, gate_keys, values, log_decay = mixer_inputs(query_pre, forget_pre, value_pre, floor_gap, H)
    start_state = jnp.zeros((H, DK, DV), jnp.float32)
    final_state, recurrent = recurrence(query_rows, gate_keys, values, log_decay, BLOCK, start_state)
    head_out = head_output(recurrent, head_gain, gate_pre)
    stream = residual_in.astype(jnp.float32) + jnp.dot(head_out, out_weight, preferred_element_type=jnp.float32)
    normed = (stream * lax.rsqrt(lax.optimization_barrier(jnp.mean(stream * stream, axis=1, keepdims=True)) + epsilon) * norm_gain).astype(jnp.bfloat16)
    up_value = jnp.dot(normed, value_weight, preferred_element_type=jnp.float32).astype(jnp.bfloat16)
    up_gate = jnp.dot(normed, gate_weight, preferred_element_type=jnp.float32).astype(jnp.bfloat16)
    zero_rows = jnp.zeros((2, up_value.shape[1]), jnp.float32)
    conv_value = causal_taps(jnp.concatenate([zero_rows, up_value.astype(jnp.float32)], axis=0), value_taps, row_count)
    conv_gate = causal_taps(jnp.concatenate([zero_rows, up_gate.astype(jnp.float32)], axis=0), gate_taps, row_count)
    hidden = (jax.nn.silu(conv_gate) * conv_value).astype(jnp.bfloat16)
    return (stream + jnp.dot(hidden, down_weight, preferred_element_type=jnp.float32)).astype(jnp.bfloat16)
```

```python
import jax
import jax.numpy as jnp
from jax import lax
from jax.sharding import PartitionSpec as P

DK = 64
SUB = 16
epsilon = 1e-06
highest = lax.Precision.HIGHEST
f32 = jnp.float32
bf16 = jnp.bfloat16


def local_recurrence(query_pre, forget_pre, value_pre, floor_gap):
    rows, width = query_pre.shape
    heads = width // DK
    subs = rows // SUB
    keys = floor_gap * jax.nn.sigmoid(-forget_pre.astype(f32))
    log_decay = jnp.log1p(-keys)
    query = jax.nn.silu(query_pre.astype(f32))
    values = value_pre.astype(f32)
    position = lax.iota(jnp.int32, rows)
    lower = (position[:, None] >= position[None, :]).astype(f32)
    running = jnp.dot(lower, log_decay, precision=highest)
    middle = running.reshape(subs, SUB, width)[:, SUB // 2 - 1, :]
    query_part = query * jnp.exp(running - jnp.repeat(middle, SUB, axis=0))
    reach = (lax.iota(jnp.int32, subs) + 1) * SUB
    seen = position[None, :, None] < reach[:, None, None]
    key_part = keys[None] * jnp.exp(
        jnp.where(seen, middle[:, None, :] - running[None], -jnp.inf)
    )
    scores = jnp.einsum(
        "ithk,ishk->hits",
        query_part.reshape(subs, SUB, heads, DK),
        key_part.reshape(subs, rows, heads, DK),
        precision=highest,
    ).reshape(heads, rows, rows)
    scores = jnp.where(position[None, :, None] >= position[None, None, :], scores, 0.0)
    value_heads = values.reshape(rows, heads, DK)
    inner = jnp.einsum("hts,shv->htv", scores, value_heads, precision=highest)
    ending = running[-1]
    state = jnp.einsum(
        "shv,shk->vhk",
        value_heads,
        (keys * jnp.exp(ending - running)).reshape(rows, heads, DK),
        precision=highest,
    ).reshape(DK, width)
    from_start = (query * jnp.exp(running)).reshape(rows, heads, DK)
    return inner, state, jnp.exp(ending), from_start


def causal_taps(before, current, taps):
    padded = jnp.concatenate([before, current], axis=1).astype(f32)
    rows = current.shape[1]
    return (
        taps[0] * padded[:, 0:rows]
        + taps[1] * padded[:, 1 : rows + 1]
        + taps[2] * padded[:, 2 : rows + 2]
    )


def on_device(
    residual_in,
    query_pre,
    forget_pre,
    value_pre,
    gate_pre,
    floor_gap,
    head_gain,
    out_weight,
    norm_gain,
    value_weight,
    gate_weight,
    value_taps,
    gate_taps,
    down_weight,
):
    sp = lax.axis_size("sp")
    tp = lax.axis_size("tp")
    inner_size = 4 if sp % 4 == 0 else 1
    outer = sp // inner_size
    me = lax.axis_index("sp")
    my_outer = me // inner_size
    my_inner = me % inner_size
    outer_groups = [[o * inner_size + i for o in range(outer)] for i in range(inner_size)]
    inner_groups = [[o * inner_size + i for i in range(inner_size)] for o in range(outer)]
    rows, my_width = residual_in.shape
    width = my_width * tp
    depth, half = value_weight.shape
    chunk = half // outer

    def exchange(array):
        return lax.all_to_all(
            array, "sp", 0, 0, axis_index_groups=outer_groups, tiled=True
        )

    def gather_inner(array):
        return lax.all_gather(array, "sp", axis_index_groups=inner_groups)

    up_pair = jnp.stack([value_weight, gate_weight]).reshape(2, depth, outer, chunk)
    up_pair = up_pair.transpose(2, 0, 1, 3)
    down_part = down_weight.reshape(outer, chunk, depth)
    up_mine = gather_inner(exchange(up_pair))
    down_mine = gather_inner(exchange(down_part))
    value_chunk = up_mine[:, :, 0].reshape(width, chunk)
    gate_chunk = up_mine[:, :, 1].reshape(width, chunk)
    down_chunk = down_mine.transpose(2, 1, 0, 3).reshape(chunk, width)

    out_full = lax.all_gather(out_weight, "tp", axis=1, tiled=True)
    gain_full = lax.all_gather(norm_gain, "tp", axis=0, tiled=True)
    residual_rows = lax.all_gather(residual_in, "tp", axis=1, tiled=True)
    residual_group = lax.all_gather(
        residual_rows, "sp", axis=0, tiled=True, axis_index_groups=outer_groups
    )

    inner, state, total_decay, from_start = local_recurrence(
        query_pre, forget_pre, value_pre, floor_gap
    )
    heads = inner.shape[0]
    packed = jnp.concatenate([state, jnp.broadcast_to(total_decay, (8, heads * DK))], axis=0)
    everyone = lax.all_gather(packed, "sp")
    entering = jnp.zeros_like(state)
    for j in range(sp - 1):
        advanced = entering * everyone[j, DK] + everyone[j, :DK]
        entering = jnp.where(j < me, advanced, entering)
    carried = jnp.einsum(
        "thk,vhk->htv", from_start, entering.reshape(DK, heads, DK), precision=highest
    )
    recurrent = (inner + carried).transpose(1, 0, 2)
    scaled = (
        recurrent
        * lax.rsqrt(jnp.mean(recurrent * recurrent, axis=-1, keepdims=True) + epsilon)
        * head_gain
    )
    gating = jax.nn.silu(gate_pre.astype(f32)).reshape(recurrent.shape)
    head_out = (scaled * gating).reshape(rows, heads * DK).astype(bf16)

    head_rows = lax.all_gather(head_out, "tp", axis=1, tiled=True)
    head_group = lax.all_gather(
        head_rows, "sp", axis=0, tiled=True, axis_index_groups=outer_groups
    )
    stream = residual_group.astype(f32) + jnp.dot(
        head_group, out_full, preferred_element_type=f32
    )
    squares = jnp.mean(stream * stream, axis=1, keepdims=True)
    normed = (stream * lax.rsqrt(squares + epsilon) * gain_full).astype(bf16)
    normed = (
        normed.reshape(outer * rows, outer, inner_size, depth)
        .transpose(0, 2, 1, 3)
        .reshape(outer * rows, width)
    )
    up_value = jnp.dot(normed, value_chunk, preferred_element_type=f32).astype(bf16)
    up_gate = jnp.dot(normed, gate_chunk, preferred_element_type=f32).astype(bf16)
    up_value = up_value.reshape(outer, rows, chunk)
    up_gate = up_gate.reshape(outer, rows, chunk)
    tails = jnp.concatenate([up_value[:, rows - 2 :], up_gate[:, rows - 2 :]], axis=2)
    pairs = [
        (o * inner_size + i, o * inner_size + (i + 1) % inner_size)
        for o in range(outer)
        for i in range(inner_size)
    ]
    arrived = lax.ppermute(tails, "sp", pairs) if inner_size > 1 else tails
    wrapped = jnp.concatenate([jnp.zeros_like(arrived[:1]), arrived[:-1]], axis=0)
    before = jnp.where(my_inner == 0, wrapped, arrived)

    my_taps = lambda taps: lax.dynamic_slice_in_dim(taps, my_outer * chunk, chunk, axis=1)
    conv_value = causal_taps(before[:, :, :chunk], up_value, my_taps(value_taps))
    conv_gate = causal_taps(before[:, :, chunk:], up_gate, my_taps(gate_taps))
    hidden = (jax.nn.silu(conv_gate) * conv_value).astype(bf16)
    terms = jnp.dot(
        hidden.reshape(outer * rows, chunk), down_chunk, preferred_element_type=f32
    ).astype(bf16)
    summed = lax.psum_scatter(
        terms, "sp", scatter_dimension=0, tiled=True, axis_index_groups=outer_groups
    )
    summed = lax.psum_scatter(summed, "tp", scatter_dimension=1, tiled=True)
    own = lax.dynamic_slice(
        stream, (my_outer * rows, lax.axis_index("tp") * my_width), (rows, my_width)
    )
    return (own + summed.astype(f32)).astype(bf16)


def solution(mesh):
    rows = P(("grp", "sp"), "tp")
    return jax.shard_map(
        on_device,
        mesh=mesh,
        in_specs=(
            rows,
            rows,
            rows,
            rows,
            rows,
            P("tp"),
            P(),
            P(None, "tp"),
            P("tp"),
            P("sp", "tp"),
            P("sp", "tp"),
            P(None, "tp"),
            P(None, "tp"),
            P("tp", "sp"),
        ),
        out_specs=rows,
        check_vma=False,
    )
```

```python
import jax
import jax.numpy as jnp
from jax import lax
from jax.sharding import PartitionSpec as P

DK = 64
SUB = 16
epsilon = 1e-06
highest = lax.Precision.HIGHEST
f32 = jnp.float32
bf16 = jnp.bfloat16


def local_recurrence(query_pre, forget_pre, value_pre, floor_gap):
    rows, width = query_pre.shape
    heads = width // DK
    subs = rows // SUB
    keys = floor_gap * jax.nn.sigmoid(-forget_pre.astype(f32))
    log_decay = jnp.log1p(-keys)
    query = jax.nn.silu(query_pre.astype(f32))
    values = value_pre.astype(f32)
    position = lax.iota(jnp.int32, rows)
    lower = (position[:, None] >= position[None, :]).astype(f32)
    running = jnp.dot(lower, log_decay, precision=highest)
    middle = running.reshape(subs, SUB, width)[:, SUB // 2 - 1, :]
    query_part = query * jnp.exp(running - jnp.repeat(middle, SUB, axis=0))
    reach = (lax.iota(jnp.int32, subs) + 1) * SUB
    seen = position[None, :, None] < reach[:, None, None]
    key_part = keys[None] * jnp.exp(
        jnp.where(seen, middle[:, None, :] - running[None], -jnp.inf)
    )
    scores = jnp.einsum(
        "ithk,ishk->hits",
        query_part.reshape(subs, SUB, heads, DK),
        key_part.reshape(subs, rows, heads, DK),
        precision=highest,
    ).reshape(heads, rows, rows)
    scores = jnp.where(position[None, :, None] >= position[None, None, :], scores, 0.0)
    value_heads = values.reshape(rows, heads, DK)
    inner = jnp.einsum("hts,shv->htv", scores, value_heads, precision=highest)
    ending = running[-1]
    state = jnp.einsum(
        "shv,shk->vhk",
        value_heads,
        (keys * jnp.exp(ending - running)).reshape(rows, heads, DK),
        precision=highest,
    ).reshape(DK, width)
    from_start = (query * jnp.exp(running)).reshape(rows, heads, DK)
    return inner, state, jnp.exp(ending), from_start


def causal_taps(before, current, taps):
    padded = jnp.concatenate([before, current], axis=1).astype(f32)
    rows = current.shape[1]
    return (
        taps[0] * padded[:, 0:rows]
        + taps[1] * padded[:, 1 : rows + 1]
        + taps[2] * padded[:, 2 : rows + 2]
    )


def on_device(
    residual_in,
    query_pre,
    forget_pre,
    value_pre,
    gate_pre,
    floor_gap,
    head_gain,
    out_weight,
    norm_gain,
    value_weight,
    gate_weight,
    value_taps,
    gate_taps,
    down_weight,
):
    sp = lax.axis_size("sp")
    tp = lax.axis_size("tp")
    inner_size = 4 if sp % 4 == 0 else 1
    outer = sp // inner_size
    me = lax.axis_index("sp")
    my_outer = me // inner_size
    my_inner = me % inner_size
    outer_groups = [[o * inner_size + i for o in range(outer)] for i in range(inner_size)]
    inner_groups = [[o * inner_size + i for i in range(inner_size)] for o in range(outer)]
    rows, my_width = residual_in.shape
    width = my_width * tp
    depth, half = value_weight.shape
    chunk = half // outer

    wide_groups = [
        [s * tp + t for s in group for t in range(tp)] for group in outer_groups
    ]

    def exchange(array):
        return lax.all_to_all(
            array, "sp", 0, 0, axis_index_groups=outer_groups, tiled=True
        )

    def gather_inner(array):
        return lax.all_gather(array, "sp", axis_index_groups=inner_groups)

    def gather_wide(array):
        gathered = lax.all_gather(array, ("sp", "tp"), axis_index_groups=wide_groups)
        gathered = gathered.reshape(outer, tp, *array.shape)
        return [gathered[:, t].reshape(-1, array.shape[1]) for t in range(tp)]

    def reorder(pieces):
        span = pieces[0].shape[-1]
        blocks = []
        for i in range(inner_size):
            for o in range(outer):
                start = (o * inner_size + i) * depth
                low = start % span
                blocks.append(pieces[start // span][..., low : low + depth])
        return lax.optimization_barrier(jnp.concatenate(blocks, axis=-1))

    up_parts = jnp.stack(
        [
            jnp.concatenate(
                [
                    value_weight[:, o * chunk : (o + 1) * chunk],
                    gate_weight[:, o * chunk : (o + 1) * chunk],
                ],
                axis=1,
            )
            for o in range(outer)
        ]
    )
    up_chunk = gather_inner(exchange(up_parts)).reshape(width, 2 * chunk)
    down_parts = down_weight.reshape(outer, chunk, depth)
    down_mine = gather_inner(exchange(down_parts))
    down_chunk = down_mine.transpose(2, 1, 0, 3).reshape(chunk, width)

    out_full = reorder(list(lax.all_gather(out_weight, "tp")))
    gain_full = reorder(list(lax.all_gather(norm_gain, "tp")))
    residual_group = reorder(gather_wide(residual_in))

    inner, state, total_decay, from_start = local_recurrence(
        query_pre, forget_pre, value_pre, floor_gap
    )
    heads = inner.shape[0]
    first = total_decay.astype(bf16)
    rest = total_decay - first.astype(f32)
    second = rest.astype(bf16)
    third = (rest - second.astype(f32)).astype(bf16)
    spare = jnp.zeros((13, heads * DK), bf16)
    packed = jnp.concatenate(
        [state.astype(bf16), first[None], second[None], third[None], spare], axis=0
    )
    everyone = lax.all_gather(packed, "sp").astype(f32)
    decays = everyone[:, DK] + everyone[:, DK + 1] + everyone[:, DK + 2]
    entering = jnp.zeros_like(state)
    for j in range(sp - 1):
        advanced = entering * decays[j] + everyone[j, :DK]
        entering = jnp.where(j < me, advanced, entering)
    carried = jnp.einsum(
        "thk,vhk->htv", from_start, entering.reshape(DK, heads, DK), precision=highest
    )
    recurrent = (inner + carried).transpose(1, 0, 2)
    scaled = (
        recurrent
        * lax.rsqrt(jnp.mean(recurrent * recurrent, axis=-1, keepdims=True) + epsilon)
        * head_gain
    )
    gating = jax.nn.silu(gate_pre.astype(f32)).reshape(recurrent.shape)
    head_out = (scaled * gating).reshape(rows, heads * DK).astype(bf16)

    head_group = jnp.concatenate(gather_wide(head_out), axis=1)
    stream = residual_group.astype(f32) + jnp.dot(
        head_group, out_full, preferred_element_type=f32
    )
    squares = jnp.mean(stream * stream, axis=1, keepdims=True)
    normed = (stream * lax.rsqrt(squares + epsilon) * gain_full).astype(bf16)
    up = jnp.dot(normed, up_chunk, preferred_element_type=f32).astype(bf16)
    up = up.reshape(outer, rows, 2 * chunk)
    tails = up[:, rows - 2 :]
    pairs = [
        (o * inner_size + i, o * inner_size + (i + 1) % inner_size)
        for o in range(outer)
        for i in range(inner_size)
    ]
    arrived = lax.ppermute(tails, "sp", pairs) if inner_size > 1 else tails
    wrapped = jnp.concatenate([jnp.zeros_like(arrived[:1]), arrived[:-1]], axis=0)
    before = jnp.where(my_inner == 0, wrapped, arrived)

    taps = jnp.concatenate(
        [
            lax.dynamic_slice_in_dim(value_taps, my_outer * chunk, chunk, axis=1),
            lax.dynamic_slice_in_dim(gate_taps, my_outer * chunk, chunk, axis=1),
        ],
        axis=1,
    )
    conv = causal_taps(before, up, taps)
    hidden = (jax.nn.silu(conv[:, :, chunk:]) * conv[:, :, :chunk]).astype(bf16)
    terms = jnp.dot(
        hidden.reshape(outer * rows, chunk), down_chunk, preferred_element_type=f32
    ).astype(bf16)
    terms = jnp.stack(
        [
            terms[:, t * my_width : (t + 1) * my_width].reshape(outer, rows, my_width)
            for t in range(tp)
        ],
        axis=1,
    )
    summed = lax.psum_scatter(
        terms.reshape(outer * tp, rows, my_width),
        ("sp", "tp"),
        scatter_dimension=0,
        axis_index_groups=wide_groups,
    )
    my_heads = lax.dynamic_slice_in_dim(head_group, my_outer * rows, rows, axis=0)
    own = residual_in.astype(f32) + jnp.dot(
        my_heads, out_weight, preferred_element_type=f32
    )
    return (own + summed.astype(f32)).astype(bf16)


def solution(mesh):
    rows = P(("grp", "sp"), "tp")
    return jax.shard_map(
        on_device,
        mesh=mesh,
        in_specs=(
            rows,
            rows,
            rows,
            rows,
            rows,
            P("tp"),
            P(),
            P(None, "tp"),
            P("tp"),
            P("sp", "tp"),
            P("sp", "tp"),
            P(None, "tp"),
            P(None, "tp"),
            P("tp", "sp"),
        ),
        out_specs=rows,
        check_vma=False,
    )
```

```python
import jax
import jax.numpy as jnp
from jax import lax
from jax.sharding import PartitionSpec as P

DK = 64
SUB = 16
epsilon = 1e-06
highest = lax.Precision.HIGHEST
f32 = jnp.float32
bf16 = jnp.bfloat16


def local_recurrence(query_pre, forget_pre, value_pre, floor_gap):
    rows, width = query_pre.shape
    heads = width // DK
    subs = rows // SUB
    keys = floor_gap * jax.nn.sigmoid(-forget_pre.astype(f32))
    log_decay = jnp.log1p(-keys)
    query = jax.nn.silu(query_pre.astype(f32))
    values = value_pre.astype(f32)
    position = lax.iota(jnp.int32, rows)
    lower = (position[:, None] >= position[None, :]).astype(f32)
    running = jnp.dot(lower, log_decay, precision=highest)
    middle = running.reshape(subs, SUB, width)[:, SUB // 2 - 1, :]
    query_part = query * jnp.exp(running - jnp.repeat(middle, SUB, axis=0))
    reach = (lax.iota(jnp.int32, subs) + 1) * SUB
    seen = position[None, :, None] < reach[:, None, None]
    key_part = keys[None] * jnp.exp(
        jnp.where(seen, middle[:, None, :] - running[None], -jnp.inf)
    )
    scores = jnp.einsum(
        "ithk,ishk->hits",
        query_part.reshape(subs, SUB, heads, DK),
        key_part.reshape(subs, rows, heads, DK),
        precision=highest,
    ).reshape(heads, rows, rows)
    scores = jnp.where(position[None, :, None] >= position[None, None, :], scores, 0.0)
    value_heads = values.reshape(rows, heads, DK)
    inner = jnp.einsum("hts,shv->htv", scores, value_heads, precision=highest)
    ending = running[-1]
    state = jnp.einsum(
        "shv,shk->vhk",
        value_heads,
        (keys * jnp.exp(ending - running)).reshape(rows, heads, DK),
        precision=highest,
    ).reshape(DK, width)
    from_start = (query * jnp.exp(running)).reshape(rows, heads, DK)
    return inner, state, jnp.exp(ending), from_start


def causal_taps(before, current, taps):
    padded = jnp.concatenate([before, current], axis=1).astype(f32)
    rows = current.shape[1]
    return (
        taps[0] * padded[:, 0:rows]
        + taps[1] * padded[:, 1 : rows + 1]
        + taps[2] * padded[:, 2 : rows + 2]
    )


def on_device(
    residual_in,
    query_pre,
    forget_pre,
    value_pre,
    gate_pre,
    floor_gap,
    head_gain,
    out_weight,
    norm_gain,
    value_weight,
    gate_weight,
    value_taps,
    gate_taps,
    down_weight,
):
    sp = lax.axis_size("sp")
    tp = lax.axis_size("tp")
    inner_size = 4 if sp % 4 == 0 else 1
    outer = sp // inner_size
    me = lax.axis_index("sp")
    my_outer = me // inner_size
    my_inner = me % inner_size
    outer_groups = [[o * inner_size + i for o in range(outer)] for i in range(inner_size)]
    inner_groups = [[o * inner_size + i for i in range(inner_size)] for o in range(outer)]
    rows, my_width = residual_in.shape
    width = my_width * tp
    depth, half = value_weight.shape
    chunk = half // outer

    wide_groups = [
        [s * tp + t for s in group for t in range(tp)] for group in outer_groups
    ]

    def exchange(array):
        return lax.all_to_all(
            array, "sp", 0, 0, axis_index_groups=outer_groups, tiled=True
        )

    def gather_inner(array):
        return lax.all_gather(array, "sp", axis_index_groups=inner_groups)

    def gather_wide(array):
        gathered = lax.all_gather(array, ("sp", "tp"), axis_index_groups=wide_groups)
        gathered = gathered.reshape(outer, tp, *array.shape)
        return [gathered[:, t].reshape(-1, array.shape[1]) for t in range(tp)]

    def reorder(pieces):
        span = pieces[0].shape[-1]
        blocks = []
        for i in range(inner_size):
            for o in range(outer):
                start = (o * inner_size + i) * depth
                low = start % span
                blocks.append(pieces[start // span][..., low : low + depth])
        return lax.optimization_barrier(jnp.concatenate(blocks, axis=-1))

    up_parts = jnp.stack(
        [
            jnp.concatenate(
                [
                    value_weight[:, o * chunk : (o + 1) * chunk],
                    gate_weight[:, o * chunk : (o + 1) * chunk],
                ],
                axis=1,
            )
            for o in range(outer)
        ]
    )
    up_chunk = gather_inner(exchange(up_parts)).reshape(width, 2 * chunk)
    down_parts = down_weight.reshape(outer, chunk, depth)
    down_mine = gather_inner(exchange(down_parts))
    down_chunk = down_mine.transpose(2, 1, 0, 3).reshape(chunk, width)

    out_full = reorder(list(lax.all_gather(out_weight, "tp")))
    gain_full = reorder(list(lax.all_gather(norm_gain, "tp")))
    residual_group = reorder(gather_wide(residual_in))

    inner, state, total_decay, from_start = local_recurrence(
        query_pre, forget_pre, value_pre, floor_gap
    )
    heads = inner.shape[0]
    first = total_decay.astype(bf16)
    rest = total_decay - first.astype(f32)
    second = rest.astype(bf16)
    third = (rest - second.astype(f32)).astype(bf16)
    spare = jnp.zeros((13, heads * DK), bf16)
    packed = jnp.concatenate(
        [state.astype(bf16), first[None], second[None], third[None], spare], axis=0
    )
    everyone = lax.all_gather(packed, "sp").astype(f32)
    decays = everyone[:, DK] + everyone[:, DK + 1] + everyone[:, DK + 2]
    entering = jnp.zeros_like(state)
    for j in range(sp - 1):
        advanced = entering * decays[j] + everyone[j, :DK]
        entering = jnp.where(j < me, advanced, entering)
    carried = jnp.einsum(
        "thk,vhk->htv", from_start, entering.reshape(DK, heads, DK), precision=highest
    )
    recurrent = (inner + carried).transpose(1, 0, 2)
    scaled = (
        recurrent
        * lax.rsqrt(jnp.mean(recurrent * recurrent, axis=-1, keepdims=True) + epsilon)
        * head_gain
    )
    gating = jax.nn.silu(gate_pre.astype(f32)).reshape(recurrent.shape)
    head_out = (scaled * gating).reshape(rows, heads * DK).astype(bf16)

    head_out, out_full = lax.optimization_barrier((head_out, out_full))
    head_group = jnp.concatenate(gather_wide(head_out), axis=1)
    stream = residual_group.astype(f32) + jnp.dot(
        head_group, out_full, preferred_element_type=f32
    )
    squares = jnp.mean(stream * stream, axis=1, keepdims=True)
    normed = (stream * lax.rsqrt(squares + epsilon) * gain_full).astype(bf16)
    up = jnp.dot(normed, up_chunk, preferred_element_type=f32).astype(bf16)
    up = up.reshape(outer, rows, 2 * chunk)
    tails = up[:, rows - 2 :]
    pairs = [
        (o * inner_size + i, o * inner_size + (i + 1) % inner_size)
        for o in range(outer)
        for i in range(inner_size)
    ]
    arrived = lax.ppermute(tails, "sp", pairs) if inner_size > 1 else tails
    wrapped = jnp.concatenate([jnp.zeros_like(arrived[:1]), arrived[:-1]], axis=0)
    before = jnp.where(my_inner == 0, wrapped, arrived)

    taps = jnp.concatenate(
        [
            lax.dynamic_slice_in_dim(value_taps, my_outer * chunk, chunk, axis=1),
            lax.dynamic_slice_in_dim(gate_taps, my_outer * chunk, chunk, axis=1),
        ],
        axis=1,
    )
    conv = causal_taps(before, up, taps)
    hidden = (jax.nn.silu(conv[:, :, chunk:]) * conv[:, :, :chunk]).astype(bf16)
    terms = jnp.dot(
        hidden.reshape(outer * rows, chunk), down_chunk, preferred_element_type=f32
    ).astype(bf16)
    summed = lax.psum_scatter(
        terms, "sp", scatter_dimension=0, tiled=True, axis_index_groups=outer_groups
    )
    summed = lax.psum_scatter(summed, "tp", scatter_dimension=1, tiled=True)
    my_heads = lax.dynamic_slice_in_dim(head_group, my_outer * rows, rows, axis=0)
    own = residual_in.astype(f32) + jnp.dot(
        my_heads, out_weight, preferred_element_type=f32
    )
    return (own + summed.astype(f32)).astype(bf16)


def solution(mesh):
    rows = P(("grp", "sp"), "tp")
    return jax.shard_map(
        on_device,
        mesh=mesh,
        in_specs=(
            rows,
            rows,
            rows,
            rows,
            rows,
            P("tp"),
            P(),
            P(None, "tp"),
            P("tp"),
            P("sp", "tp"),
            P("sp", "tp"),
            P(None, "tp"),
            P(None, "tp"),
            P("tp", "sp"),
        ),
        out_specs=rows,
        check_vma=False,
    )
```
